32 devices in a mesh: ep: 4 (over y, x), tp: 8 (over z, core).
Axes of the slice: x: 2, y: 2, z: 4, core: 2. Of those that a mesh axis runs over, the one named last changes fastest.
Arguments:
- mix_tokens: bfloat16 [4096, 2048], P(('ep', 'tp')), may hold values from -6 to 6
- mix_gain: bfloat16 [2048], replicated, may hold values from 0.099609375 to 1.8984375
- gate_proj: bfloat16 [2048, 1024], P(None, 'tp'), may hold values from -0.125 to 0.125
- conv_proj: bfloat16 [2048, 1024], P(None, 'tp'), may hold values from -0.125 to 0.125
- value_proj: bfloat16 [2048, 1024], P(None, 'tp'), may hold values from -0.125 to 0.125
- conv_taps: bfloat16 [3, 1024], P(None, 'tp'), may hold values from -3 to 3
- out_proj: bfloat16 [1024, 2048], P('tp'), may hold values from -0.1875 to 0.1875
- moe_tokens: bfloat16 [2048, 2048], P(('ep', 'tp')), may hold values from -6 to 6
- moe_gain: bfloat16 [2048], replicated, may hold values from 0.099609375 to 1.8984375
- expert_ids: int32 [2048, 2], P(('ep', 'tp')), may hold values from 0 to 3, all different within a row; in each aligned block of 64 rows (0 to 63, 64 to 127, ...) at most 36 rows name the same one
- expert_scores: float32 [2048, 2], P(('ep', 'tp')), may hold values from -6 to 6
- expert_gate: bfloat16 [4, 2048, 4096], P('ep', None, 'tp'), may hold values from -0.125 to 0.125
- expert_up: bfloat16 [4, 2048, 4096], P('ep', None, 'tp'), may hold values from -0.125 to 0.125
- expert_down: bfloat16 [4, 4096, 2048], P('ep', 'tp'), may hold values from -0.09375 to 0.09375
Outputs:
- mix_out: bfloat16 [4096, 2048], P(('ep', 'tp'))
- moe_out: bfloat16 [2048, 2048], P(('ep', 'tp'))
The draws below stay inside these ranges and needn't reach their ends.
Inputs may be any that keep to these rules, and one draw needn't show every extreme that they name: `expert_ids`: each row names 2 different experts; among the rows of one device no expert is named more than 36 times.
All inputs are finite; a program needn't handle non-finite values.
Results may differ from the reference program's by a relative error of at most 0.018.
Values may be sent and summed in bfloat16 or wider, within the bound.
No kernel may reach another device: no remote copies, remote signals or barrier semaphores. Data moves between devices by JAX's collectives and lax.ppermute only.
A program may use at most 128 MiB of HBM per device.

```python
import math
import jax
import jax.numpy as jnp
import numpy as np
from jax import lax

D = 2048
CONV = 1024
FF = 4096
TAPS = 3
TOP = 2
MOE_DEV = 64
EXPERTS = 4
CAP = 36
MIX_TOKENS = 4096
MOE_TOKENS = 2048
N_EP = 4
N_TP = 8


def shard_levels(own_key, dims, shards, low, high):
    gain, own = 1.0, jax.random.fold_in(own_key, 6)
    for dim, blocks in shards:
        draws = jnp.exp(jax.random.uniform(jax.random.fold_in(own, dim), (blocks,), jnp.float32, low / len(shards), high / len(shards)))
        gain = gain * jnp.repeat(draws, dims[dim] // blocks).reshape([-1 if axis == dim else 1 for axis in range(len(dims))])
    return gain


def deal_out(key, own, number, rows, count, top, most, lean):
    order = jax.random.permutation(key, count)
    crowded, ordinary = shares(count, rows * top, most, lean, True), shares(count, rows * top, most, lean, False)
    places = jnp.arange(count)

    def named(tallies, rotation):
        used = int((tallies > 0).sum())
        fixed = max(1, used // 4)
        shifted = fixed + (places - fixed + rotation * (used - fixed)) % max(1, count - fixed)
        return jnp.zeros((count,), jnp.int32).at[order[jnp.where(places < fixed, places, shifted)]].set(jnp.asarray(tallies, jnp.int32))

    tallies = jnp.where(number % 4 == 0, named(crowded, number // 4), named(ordinary, number - number // 4 - 1))
    mixed = jax.random.permutation(jax.random.fold_in(own, 3), count)
    donor, taker = mixed[0:count // 2 * 2:2], mixed[1:count // 2 * 2:2]
    room = jnp.minimum(tallies[donor] - 1, most - tallies[taker]) // 2
    room = jnp.where((donor == order[0]) | (taker == order[0]) | (tallies[taker] == 0), 0, jnp.maximum(room, 0))
    shifted = jax.random.randint(jax.random.fold_in(own, 4), (count // 2,), 0, 1 << 20) % (room + 1)
    tallies = tallies.at[donor].add(-shifted).at[taker].add(shifted)
    labels = jnp.searchsorted(jnp.cumsum(tallies), jnp.arange(rows * top), side="right").astype(jnp.int32)
    listing = labels.reshape(top, rows).T
    listing = listing[jax.random.permutation(jax.random.fold_in(own, 1), rows)]
    rotation = jax.random.randint(jax.random.fold_in(own, 2), (rows, 1), 0, top)
    return jnp.take_along_axis(listing, (jnp.arange(top)[None, :] + rotation) % top, axis=1)


def shares(number_of, total, most, slope, full):
    loads = [(1 << 20) // math.isqrt(standing ** slope) + 1 for standing in range(1, number_of + 1)]
    largest = most if full else min(most, max(-(-total // number_of), total * loads[0] // sum(loads)))
    least = 1 if total - largest >= number_of - 1 else 0
    given, surplus = [largest] + [least] * (number_of - 1), total - largest - least * (number_of - 1)
    while surplus > 0:
        candidates = [i for i in range(1, number_of) if given[i] < largest] or [i for i in range(1, number_of) if given[i] < most]
        mass, budget = sum([loads[i] for i in candidates]), surplus
        for i in candidates:
            addition = min(most - given[i], max(1, budget * loads[i] // mass), surplus)
            given[i] = given[i] + addition
            surplus = surplus - addition
    return np.array(given)


def centred(own_key, extent, spread, reach, split=(), kind=jnp.bfloat16):
    values = jax.random.normal(own_key, extent, jnp.float32) * spread
    if len(split) > 0:
        values = shard_levels(own_key, extent, split, -0.22, 0.18) * values
    return jnp.clip(values, min=-reach, max=reach).astype(kind)


def setup_inputs(seed: int = 0) -> dict:
    keys = jax.random.split(jax.random.key(seed), 15)
    mix_tokens = centred(keys[0], (MIX_TOKENS, D), 1.0, 6.0, ((0, 32),))
    mix_gain = jnp.clip(1.0 + 0.18 * jax.random.normal(keys[1], (D,), jnp.float32), 0.099609375, 1.8984375).astype(jnp.bfloat16)
    gate_proj = centred(keys[2], (D, CONV), D ** -0.5, 0.125, ((1, 8),))
    conv_proj = centred(keys[3], (D, CONV), D ** -0.5, 0.125, ((1, 8),))
    value_proj = centred(keys[4], (D, CONV), D ** -0.5, 0.125, ((1, 8),))
    conv_taps = centred(keys[5], (TAPS, CONV), 0.577, 3.0, ((1, 8),))
    out_proj = centred(keys[6], (CONV, D), CONV ** -0.5, 0.1875, ((0, 8),))
    moe_tokens = centred(keys[7], (MOE_TOKENS, D), 1.0, 6.0, ((0, 32),))
    moe_gain = jnp.clip(1.0 + 0.18 * jax.random.normal(keys[8], (D,), jnp.float32), 0.099609375, 1.8984375).astype(jnp.bfloat16)
    expert_ids_keys = jax.random.split(jax.random.fold_in(keys[9], 1), MOE_TOKENS // MOE_DEV)
    expert_ids_turns = jax.random.permutation(jax.random.fold_in(keys[9], 3), MOE_TOKENS // MOE_DEV)
    expert_ids = jax.vmap(lambda own, number: deal_out(jax.random.fold_in(keys[9], 2), own, number, MOE_DEV, EXPERTS, TOP, CAP, 2))(expert_ids_keys, expert_ids_turns).reshape((MOE_TOKENS, TOP))
    expert_scores = centred(keys[10], (MOE_TOKENS, TOP), 1.0, 6.0, ((0, 32),), jnp.float32)
    expert_gate = centred(keys[11], (EXPERTS, D, FF), D ** -0.5, 0.125, ((0, 4), (2, 8)))
    expert_up = centred(keys[12], (EXPERTS, D, FF), D ** -0.5, 0.125, ((0, 4), (2, 8)))
    expert_down = centred(keys[13], (EXPERTS, FF, D), FF ** -0.5, 0.09375, ((0, 4), (1, 8)))
    return {"mix_tokens": mix_tokens, "mix_gain": mix_gain, "gate_proj": gate_proj, "conv_proj": conv_proj, "value_proj": value_proj, "conv_taps": conv_taps, "out_proj": out_proj, "moe_tokens": moe_tokens, "moe_gain": moe_gain, "expert_ids": expert_ids, "expert_scores": expert_scores, "expert_gate": expert_gate, "expert_up": expert_up, "expert_down": expert_down}


norm_eps = 1e-06

def scaled_norm(row_data, gain_vec):
    values = row_data.astype(jnp.float32)
    inverse = lax.rsqrt(lax.optimization_barrier(jnp.mean(values * values, axis=1, keepdims=True)) + norm_eps)
    return (values * inverse * gain_vec.astype(jnp.float32)).astype(jnp.bfloat16)

def reference(mix_tokens, mix_gain, gate_proj, conv_proj, value_proj, conv_taps, out_proj, moe_tokens, moe_gain, expert_ids, expert_scores, expert_gate, expert_up, expert_down):
    normed = scaled_norm(mix_tokens, mix_gain)
    out_gate = jnp.dot(normed, gate_proj, preferred_element_type=jnp.float32).astype(jnp.bfloat16)
    in_gate = jnp.dot(normed, conv_proj, preferred_element_type=jnp.float32).astype(jnp.bfloat16)
    values = jnp.dot(normed, value_proj, preferred_element_type=jnp.float32).astype(jnp.bfloat16)
    signal = (in_gate.astype(jnp.float32) * values.astype(jnp.float32)).astype(jnp.bfloat16)
    length = signal.shape[0]
    padded = jnp.concatenate([jnp.zeros((TAPS - 1, CONV), jnp.bfloat16), signal], axis=0)
    tap_values = conv_taps.astype(jnp.float32)
    convolved = jnp.zeros((length, CONV), jnp.float32)
    for offset in range(TAPS):
        convolved = convolved + padded[offset:offset + length].astype(jnp.float32) * tap_values[offset]
    carried = (out_gate.astype(jnp.float32) * convolved).astype(jnp.bfloat16)
    mix_out = jnp.dot(carried, out_proj, preferred_element_type=jnp.float32).astype(jnp.bfloat16)
    moe_normed = scaled_norm(moe_tokens, moe_gain)
    flat_ids = expert_ids.reshape(-1).astype(jnp.int32)
    assigned = flat_ids.shape[0]
    bound = N_EP * N_TP * CAP
    onehot = (flat_ids[:, None] == jnp.arange(EXPERTS, dtype=jnp.int32)[None, :]).astype(jnp.int32)
    slot_rank = lax.optimization_barrier(jnp.sum((jnp.cumsum(onehot, axis=0) - onehot) * onehot, axis=1)).astype(jnp.int32)
    owner = (jnp.arange(assigned, dtype=jnp.int32) // TOP).astype(jnp.int32)
    table = jnp.zeros((EXPERTS, bound), jnp.int32).at[flat_ids, slot_rank].set(owner)
    hidden_block = FF // N_TP

    def one_expert(expert_index):
        chosen = moe_normed[table[expert_index]]
        gate_value = jnp.dot(chosen, expert_gate[expert_index], preferred_element_type=jnp.float32)
        up_value = jnp.dot(chosen, expert_up[expert_index], preferred_element_type=jnp.float32)
        hidden = (jax.nn.silu(gate_value) * up_value).astype(jnp.bfloat16)
        down = expert_down[expert_index]

        def add_block(block_index, running):
            start = (block_index * hidden_block).astype(jnp.int32)
            part_hidden = lax.dynamic_slice_in_dim(hidden, start, hidden_block, 1)
            part_weight = lax.dynamic_slice_in_dim(down, start, hidden_block, 0)
            term = jnp.dot(part_hidden, part_weight, preferred_element_type=jnp.float32).astype(jnp.bfloat16)
            term = lax.optimization_barrier(term)
            return running + term.astype(jnp.float32)
        running = lax.fori_loop(0, N_TP, add_block, jnp.zeros((bound, D), jnp.float32))
        return running.astype(jnp.bfloat16)
    results = lax.map(one_expert, jnp.arange(EXPERTS, dtype=jnp.int32))
    picked = results[flat_ids, slot_rank].reshape(-1, TOP, D)
    route_weight = jax.nn.softmax(expert_scores.astype(jnp.float32), axis=1)
    moe_out = lax.optimization_barrier(jnp.sum(route_weight[:, :, None] * picked.astype(jnp.float32), axis=1)).astype(jnp.bfloat16)
    return (mix_out, moe_out)
```

```python
import jax
import jax.numpy as jnp
from jax import lax
from jax.sharding import PartitionSpec as P

norm_eps = 1e-06


def scaled_norm(row_data, gain_vec):
    values = row_data.astype(jnp.float32)
    inverse = lax.rsqrt(jnp.mean(values * values, axis=1, keepdims=True) + norm_eps)
    return (values * inverse * gain_vec.astype(jnp.float32)).astype(jnp.bfloat16)


def shards(
    mix_tokens,
    mix_gain,
    gate_proj,
    conv_proj,
    value_proj,
    conv_taps,
    out_proj,
    moe_tokens,
    moe_gain,
    expert_ids,
    expert_scores,
    expert_gate,
    expert_up,
    expert_down,
):
    n_ep = lax.axis_size("ep")
    n_tp = lax.axis_size("tp")
    half = n_tp // 2
    ep_index = lax.axis_index("ep")
    channels = gate_proj.shape[1]
    halves = [list(range(half)), list(range(half, n_tp))]
    joint = jnp.concatenate([gate_proj, conv_proj, value_proj], axis=1)
    swap = [(t, t ^ half) for t in range(n_tp)]

    def own_piece(array):
        rows = array.shape[0] // n_ep
        return lax.ppermute(
            lax.dynamic_slice_in_dim(array, ep_index * rows, rows, 0), "tp", swap
        )

    def assembled(piece, array):
        rows = array.shape[0] // n_ep
        whole = lax.dynamic_update_slice_in_dim(
            jnp.zeros_like(array), piece, ep_index * rows, 0
        )
        for k in range(1, n_ep):
            arrived_piece = lax.ppermute(piece, "ep", [(e, e ^ k) for e in range(n_ep)])
            whole = lax.dynamic_update_slice_in_dim(
                whole, arrived_piece, (ep_index ^ k) * rows, 0
            )
        return whole

    joint_piece = own_piece(joint)
    out_piece = own_piece(out_proj)
    other_taps = lax.ppermute(conv_taps, "tp", swap)
    normed = scaled_norm(mix_tokens, mix_gain)
    moe_normed = scaled_norm(moe_tokens, moe_gain)
    normed, moe_normed = lax.optimization_barrier((normed, moe_normed))
    gathered = lax.all_gather(normed, "tp", axis=0, tiled=True, axis_index_groups=halves)
    experts = expert_gate.shape[0] * lax.axis_size("ep")
    row_count, top_count = expert_ids.shape
    capacity = top_count * row_count // experts + max(1, top_count * row_count // (8 * experts))
    width_model = moe_tokens.shape[1]
    flat_ids = expert_ids.reshape(-1)
    onehot = (flat_ids[:, None] == jnp.arange(experts, dtype=jnp.int32)[None, :]).astype(jnp.int32)
    slot_rank = jnp.sum((jnp.cumsum(onehot, axis=0) - onehot) * onehot, axis=1)
    slot_index = flat_ids * capacity + slot_rank
    slot_match = slot_index[:, None] == jnp.arange(experts * capacity, dtype=jnp.int32)[None, :]
    dispatch_map = jnp.any(
        slot_match.reshape(row_count, top_count, experts * capacity), axis=1
    ).astype(jnp.bfloat16)
    outgoing = lax.dot_general(
        dispatch_map, moe_normed, (((0,), (0,)), ((), ())), preferred_element_type=jnp.float32
    ).astype(jnp.bfloat16)
    arrived = lax.all_to_all(
        outgoing.reshape(experts, capacity, width_model),
        "ep",
        split_axis=0,
        concat_axis=0,
        tiled=True,
    )
    arrived_rows = arrived.reshape(-1, width_model)
    arrived_rows, gathered, joint_piece, out_piece, other_taps = lax.optimization_barrier(
        (arrived_rows, gathered, joint_piece, out_piece, other_taps)
    )
    portion = lax.all_gather(arrived_rows, "tp", axis=0, tiled=True)
    other_joint = assembled(joint_piece, joint)
    other_out = assembled(out_piece, out_proj)
    own_values = jnp.dot(gathered, joint, preferred_element_type=jnp.float32).astype(jnp.bfloat16)
    other_values = jnp.dot(gathered, other_joint, preferred_element_type=jnp.float32).astype(
        jnp.bfloat16
    )
    out_gate, in_gate, values = (
        jnp.concatenate(
            [part[:, index * channels : (index + 1) * channels] for part in (own_values, other_values)],
            axis=1,
        )
        for index in range(3)
    )
    signal = (in_gate.astype(jnp.float32) * values.astype(jnp.float32)).astype(jnp.bfloat16)
    tap_count = conv_taps.shape[0]
    length = signal.shape[0]
    tail = signal[length - (tap_count - 1) :]
    tail = jnp.concatenate([tail[:, channels:], tail[:, :channels]], axis=1)
    steps = [
        (device, device + half) for device in range(n_ep * n_tp - half)
    ]
    before = lax.ppermute(tail, ("ep", "tp"), steps)
    extended = jnp.concatenate([before, signal], axis=0)
    tap_values = jnp.concatenate([conv_taps, other_taps], axis=1).astype(jnp.float32)
    convolved = jnp.zeros((length, 2 * channels), jnp.float32)
    for offset in range(tap_count):
        convolved = (
            convolved + extended[offset : offset + length].astype(jnp.float32) * tap_values[offset]
        )
    carried = (out_gate.astype(jnp.float32) * convolved).astype(jnp.bfloat16)
    out_weights = jnp.concatenate([out_proj, other_out], axis=0)
    mix_partial = jnp.dot(carried, out_weights, preferred_element_type=jnp.float32).astype(
        jnp.bfloat16
    )
    portion, mix_partial = lax.optimization_barrier((portion, mix_partial))
    mix_out = lax.psum_scatter(
        mix_partial, "tp", scatter_dimension=0, tiled=True, axis_index_groups=halves
    )
    w_gate = expert_gate[0]
    w_up = expert_up[0]
    w_down = expert_down[0]
    gate_value = jnp.dot(portion, w_gate, preferred_element_type=jnp.float32)
    up_value = jnp.dot(portion, w_up, preferred_element_type=jnp.float32)
    hidden = (jax.nn.silu(gate_value) * up_value).astype(jnp.bfloat16)
    moe_partial = jnp.dot(hidden, w_down, preferred_element_type=jnp.float32).astype(jnp.bfloat16)
    moe_partial, mix_out = lax.optimization_barrier((moe_partial, mix_out))
    summed = lax.psum_scatter(moe_partial, "tp", scatter_dimension=0, tiled=True)
    returned = lax.all_to_all(
        summed.reshape(experts, capacity, width_model),
        "ep",
        split_axis=0,
        concat_axis=0,
        tiled=True,
    )
    flat_back = returned.reshape(experts * capacity, width_model)
    picked = flat_back[slot_index].reshape(row_count, top_count, width_model)
    route_weight = jax.nn.softmax(expert_scores, axis=1)
    moe_out = jnp.sum(route_weight[:, :, None] * picked.astype(jnp.float32), axis=1).astype(
        jnp.bfloat16
    )
    return (mix_out, moe_out)


def solution(mesh):
    in_specs = (
        P(("ep", "tp"), None),
        P(),
        P(None, "tp"),
        P(None, "tp"),
        P(None, "tp"),
        P(None, "tp"),
        P("tp", None),
        P(("ep", "tp"), None),
        P(),
        P(("ep", "tp"), None),
        P(("ep", "tp"), None),
        P("ep", None, "tp"),
        P("ep", None, "tp"),
        P("ep", "tp", None),
    )
    out_specs = (P(("ep", "tp"), None), P(("ep", "tp"), None))
    return jax.shard_map(shards, mesh=mesh, in_specs=in_specs, out_specs=out_specs, check_vma=False)
```

```python
import jax
import jax.numpy as jnp
from jax import lax
from jax.sharding import PartitionSpec as P

norm_eps = 1e-06


def scaled_norm(row_data, gain_vec):
    values = row_data.astype(jnp.float32)
    inverse = lax.rsqrt(jnp.mean(values * values, axis=1, keepdims=True) + norm_eps)
    return (values * inverse * gain_vec.astype(jnp.float32)).astype(jnp.bfloat16)


def shards(
    mix_tokens,
    mix_gain,
    gate_proj,
    conv_proj,
    value_proj,
    conv_taps,
    out_proj,
    moe_tokens,
    moe_gain,
    expert_ids,
    expert_scores,
    expert_gate,
    expert_up,
    expert_down,
):
    n_ep = lax.axis_size("ep")
    n_tp = lax.axis_size("tp")
    half = n_tp // 2
    ep_index = lax.axis_index("ep")
    channels = gate_proj.shape[1]
    halves = [list(range(half)), list(range(half, n_tp))]
    joint = jnp.concatenate([gate_proj, conv_proj, value_proj], axis=1)
    swap = [(t, t ^ half) for t in range(n_tp)]

    def own_rows(array):
        rows = array.shape[0] // n_ep
        return lax.dynamic_slice_in_dim(array, ep_index * rows, rows, 0)

    def assembled(piece, array):
        rows = array.shape[0] // n_ep
        whole = lax.dynamic_update_slice_in_dim(
            jnp.zeros_like(array), piece, ep_index * rows, 0
        )
        for k in range(1, n_ep):
            arrived_piece = lax.ppermute(piece, "ep", [(e, e ^ k) for e in range(n_ep)])
            whole = lax.dynamic_update_slice_in_dim(
                whole, arrived_piece, (ep_index ^ k) * rows, 0
            )
        return whole

    joint_rows = jnp.concatenate(
        [own_rows(array) for array in (gate_proj, conv_proj, value_proj)], axis=1
    )
    joint_rows, out_rows, moe_tokens = lax.optimization_barrier(
        (joint_rows, own_rows(out_proj), moe_tokens)
    )
    joint_piece = lax.ppermute(joint_rows, "tp", swap)
    out_piece = lax.ppermute(out_rows, "tp", swap)
    other_taps = lax.ppermute(conv_taps, "tp", swap)
    normed = scaled_norm(mix_tokens, mix_gain)
    moe_normed = scaled_norm(moe_tokens, moe_gain)
    experts = expert_gate.shape[0] * lax.axis_size("ep")
    row_count, top_count = expert_ids.shape
    capacity = top_count * row_count // experts + max(1, top_count * row_count // (8 * experts))
    width_model = moe_tokens.shape[1]
    flat_ids = expert_ids.reshape(-1)
    onehot = (flat_ids[:, None] == jnp.arange(experts, dtype=jnp.int32)[None, :]).astype(jnp.int32)
    slot_rank = jnp.sum((jnp.cumsum(onehot, axis=0) - onehot) * onehot, axis=1)
    slot_index = flat_ids * capacity + slot_rank
    slot_match = slot_index[:, None] == jnp.arange(experts * capacity, dtype=jnp.int32)[None, :]
    dispatch_map = jnp.any(
        slot_match.reshape(row_count, top_count, experts * capacity), axis=1
    ).astype(jnp.bfloat16)
    outgoing = lax.dot_general(
        dispatch_map, moe_normed, (((0,), (0,)), ((), ())), preferred_element_type=jnp.float32
    ).astype(jnp.bfloat16)
    arrived = lax.all_to_all(
        outgoing.reshape(experts, capacity, width_model),
        "ep",
        split_axis=0,
        concat_axis=0,
        tiled=True,
    )
    arrived_rows = arrived.reshape(-1, width_model)
    arrived_rows, joint_piece, out_piece, other_taps = lax.optimization_barrier(
        (arrived_rows, joint_piece, out_piece, other_taps)
    )
    portion = lax.all_gather(arrived_rows, "tp", axis=0, tiled=True)
    other_joint = assembled(joint_piece, joint)
    other_out = assembled(out_piece, out_proj)
    portion, other_joint, other_out, other_taps, joint = lax.optimization_barrier(
        (portion, other_joint, other_out, other_taps, joint)
    )
    gathered = lax.all_gather(normed, "tp", axis=0, tiled=True, axis_index_groups=halves)
    w_gate = expert_gate[0]
    w_up = expert_up[0]
    w_down = expert_down[0]
    gate_value = jnp.dot(portion, w_gate, preferred_element_type=jnp.float32)
    up_value = jnp.dot(portion, w_up, preferred_element_type=jnp.float32)
    hidden = (jax.nn.silu(gate_value) * up_value).astype(jnp.bfloat16)
    moe_partial = jnp.dot(hidden, w_down, preferred_element_type=jnp.float32).astype(jnp.bfloat16)
    gathered, _ = lax.optimization_barrier((gathered, moe_partial))
    own_values = jnp.dot(gathered, joint, preferred_element_type=jnp.float32).astype(jnp.bfloat16)
    other_values = jnp.dot(gathered, other_joint, preferred_element_type=jnp.float32).astype(
        jnp.bfloat16
    )
    out_gate, in_gate, values = (
        jnp.concatenate(
            [part[:, index * channels : (index + 1) * channels] for part in (own_values, other_values)],
            axis=1,
        )
        for index in range(3)
    )
    signal = (in_gate.astype(jnp.float32) * values.astype(jnp.float32)).astype(jnp.bfloat16)
    tap_count = conv_taps.shape[0]
    length = signal.shape[0]
    tail = signal[length - (tap_count - 1) :]
    tail = jnp.concatenate([tail[:, channels:], tail[:, :channels]], axis=1)
    steps = [
        (device, device + half) for device in range(n_ep * n_tp - half)
    ]
    before = lax.ppermute(tail, ("ep", "tp"), steps)
    extended = jnp.concatenate([before, signal], axis=0)
    tap_values = jnp.concatenate([conv_taps, other_taps], axis=1).astype(jnp.float32)
    convolved = jnp.zeros((length, 2 * channels), jnp.float32)
    for offset in range(tap_count):
        convolved = (
            convolved + extended[offset : offset + length].astype(jnp.float32) * tap_values[offset]
        )
    carried = (out_gate.astype(jnp.float32) * convolved).astype(jnp.bfloat16)
    out_weights = jnp.concatenate([out_proj, other_out], axis=0)
    mix_partial = jnp.dot(carried, out_weights, preferred_element_type=jnp.float32).astype(
        jnp.bfloat16
    )
    summed = lax.psum_scatter(moe_partial, "tp", scatter_dimension=0, tiled=True)
    mix_partial, summed = lax.optimization_barrier((mix_partial, summed))
    mix_out = lax.psum_scatter(
        mix_partial, "tp", scatter_dimension=0, tiled=True, axis_index_groups=halves
    )
    returned = lax.all_to_all(
        summed.reshape(experts, capacity, width_model),
        "ep",
        split_axis=0,
        concat_axis=0,
        tiled=True,
    )
    flat_back = returned.reshape(experts * capacity, width_model)
    picked = flat_back[slot_index].reshape(row_count, top_count, width_model)
    route_weight = jax.nn.softmax(expert_scores, axis=1)
    moe_out = jnp.sum(route_weight[:, :, None] * picked.astype(jnp.float32), axis=1).astype(
        jnp.bfloat16
    )
    return (mix_out, moe_out)


def solution(mesh):
    in_specs = (
        P(("ep", "tp"), None),
        P(),
        P(None, "tp"),
        P(None, "tp"),
        P(None, "tp"),
        P(None, "tp"),
        P("tp", None),
        P(("ep", "tp"), None),
        P(),
        P(("ep", "tp"), None),
        P(("ep", "tp"), None),
        P("ep", None, "tp"),
        P("ep", None, "tp"),
        P("ep", "tp", None),
    )
    out_specs = (P(("ep", "tp"), None), P(("ep", "tp"), None))

    return jax.shard_map(shards, mesh=mesh, in_specs=in_specs, out_specs=out_specs, check_vma=False)
```
